32 devices in a mesh: grp: 2 (over y), sp: 4 (over z), tp: 4 (over x, core).
Axes of the slice: x: 2, y: 2, z: 4, core: 2. Of those that a mesh axis runs over, the one named last changes fastest.
Arguments:
- conv_value: bfloat16 [4096, 1024], P(('grp', 'sp'), 'tp'), parts along dimension 0, may hold values from -6 to 6
- conv_gate: bfloat16 [4096, 1024], P(('grp', 'sp'), 'tp'), parts along dimension 0, may hold values from -6 to 6
- kernel: bfloat16 [31, 1024], P(None, 'tp'), may hold values from -4 to 4
- conv_bias: float32 [1024], P('tp'), may hold values from -3 to 3
- ln_gain: float32 [1024], P('tp'), may hold values from 0.1 to 1.9
- ln_bias: float32 [1024], P('tp'), may hold values from -3 to 3
- out_gain: float32 [1024], P('tp'), may hold values from 0.1 to 1.9
- out_weight: bfloat16 [1024, 2048], replicated, may hold values from -0.1875 to 0.1875
- residual: bfloat16 [4096, 2048], P(('grp', 'sp', 'tp')), parts along dimension 0, may hold values from -6 to 6
- moe_gain: float32 [2048], replicated, may hold values from 0.1 to 1.9
- expert_ids: int32 [4096, 2], P(('grp', 'sp', 'tp')), parts along dimension 0, may hold values from 0 to 15, as said below
- expert_weights: float32 [4096, 2], P(('grp', 'sp', 'tp')), parts along dimension 0, may hold values from 0.1 to 0.7
- w_gate: bfloat16 [16, 2048, 512], P(('sp', 'tp')), may hold values from -0.125 to 0.125
- w_up: bfloat16 [16, 2048, 512], P(('sp', 'tp')), may hold values from -0.125 to 0.125
- w_down: bfloat16 [16, 512, 2048], P(('sp', 'tp')), may hold values from -0.25 to 0.25
Outputs:
- layer_out: bfloat16 [4096, 2048], P(('grp', 'sp', 'tp')), parts along dimension 0
The draws below stay inside these ranges and needn't reach their ends.
There are 2 independent parts, one for each index of `grp`. The reference program is written for one: setup_inputs(seed, part) draws one part's arguments, and reference() takes and returns one part's arrays. A program takes and returns all parts, laid end to end along the dimension named above; an argument that names none is the same for every part. Nothing has to cross between parts.
Inputs may be any that keep to these rules, and one draw needn't show every extreme that they name: `expert_ids`: each row names two different experts of one group (group = expert number // 4). Among the 128 rows of one device (aligned blocks of 128 rows) no expert is named more than 32 times, and in every such block some expert is named exactly 32 times.
All inputs are finite; a program needn't handle non-finite values.
Results may differ from the reference program's by a relative error of at most 0.0095.
Values may be sent and summed in bfloat16 or wider, within the bound.
A program may use at most 64 MiB of HBM per device.

```python
import jax
import jax.numpy as jnp
from jax import lax

D = 2048
CONV_CH = 1024
KERNEL = 31
HID = 512
ROWS = 128
TOKENS = 2048
EXPERTS = 16
EPG = 4
CAP = 32


def draw_kernel(key, part):
    key_base, key_jitter = jax.random.split(jax.random.fold_in(key, 11))
    ramp = jnp.exp(jnp.log(0.3) + jnp.log(10.0) * jnp.arange(CONV_CH, dtype=jnp.float32) / CONV_CH)
    jitter = jnp.exp(jax.random.uniform(key_jitter, (CONV_CH,), jnp.float32, -0.35, 0.35))
    base = jnp.clip(jax.random.normal(key_base, (KERNEL, CONV_CH), jnp.float32), -4.0, 4.0)
    return (base * ramp * jitter / jnp.sqrt(jnp.float32(KERNEL))).astype(jnp.bfloat16)


def draw_expert_ids(key, part):
    group_size = min(ROWS, EXPERTS // 2)
    rounds = TOKENS // group_size
    busiest = jax.random.randint(jax.random.fold_in(key, 21), (), 0, EXPERTS)
    round_keys = jax.random.split(jax.random.fold_in(key, 22), rounds)
    numbers = jnp.arange(EXPERTS, dtype=jnp.int32)

    def one_round(round_key):
        key_shift, key_order, key_mix, key_swap = jax.random.split(round_key, 4)
        shift_by = jax.random.randint(key_shift, (), 1, EPG)
        pre_image = busiest // EPG * EPG + (busiest % EPG - shift_by) % EPG
        scores = jax.random.permutation(key_order, EXPERTS).astype(jnp.int32)
        forced = (numbers == busiest) | (numbers == pre_image)
        scores = jnp.where(forced, scores + EXPERTS, scores)
        _, chosen = lax.top_k(scores, group_size)
        chosen = jax.random.permutation(key_mix, chosen.astype(jnp.int32))
        second = chosen // EPG * EPG + (chosen % EPG + shift_by) % EPG
        swapped = jax.random.randint(key_swap, (group_size,), 0, 2)
        first_col = jnp.where(swapped == 1, second, chosen)
        second_col = jnp.where(swapped == 1, chosen, second)
        return jnp.stack([first_col, second_col], axis=1).astype(jnp.int32)
    return jax.vmap(one_round)(round_keys).reshape(TOKENS, 2).astype(jnp.int32)


def block_levels(own_key, extent, shards, low, largest):
    def one(dim, shards_of):
        steps = jax.random.uniform(jax.random.fold_in(jax.random.fold_in(own_key, 6), dim), (shards_of,), jnp.float32, low / len(shards), largest / len(shards))
        return jnp.repeat(jnp.exp(steps), extent[dim] // shards_of).reshape((-1,) + (1,) * (len(extent) - dim - 1))

    level = one(*shards[0])
    for cut in shards[1:]:
        level = level * one(*cut)
    return level


def noise(stream_key, extent, scale, bound, shards=(), kind=jnp.bfloat16):
    array = scale * jax.random.normal(stream_key, extent, jnp.float32)
    if shards:
        array = array * block_levels(stream_key, extent, shards, -0.22, 0.18)
    return jnp.clip(array, -bound, bound).astype(kind)


def setup_inputs(seed: int = 0, part: int = 0) -> dict:
    keys = jax.random.split(jax.random.key(seed), 16)
    own_keys = jax.random.split(jax.random.fold_in(keys[15], part), 16)
    conv_value = noise(own_keys[0], (TOKENS, CONV_CH), 1.0, 6.0, ((0, 4), (1, 4)))
    conv_gate = noise(own_keys[1], (TOKENS, CONV_CH), 1.0, 6.0, ((0, 4), (1, 4)))
    kernel = draw_kernel(jax.random.fold_in(keys[15], 71), part)
    conv_bias = noise(keys[3], (CONV_CH,), 0.5, 3.0, ((0, 4),), jnp.float32)
    ln_gain = jnp.clip(1.0 + 0.18 * jax.random.normal(keys[4], (CONV_CH,), jnp.float32), 0.1, 1.9)
    ln_bias = noise(keys[5], (CONV_CH,), 0.5, 3.0, ((0, 4),), jnp.float32)
    out_gain = jnp.clip(1.0 + 0.18 * jax.random.normal(keys[6], (CONV_CH,), jnp.float32), 0.1, 1.9)
    out_weight = noise(keys[7], (CONV_CH, D), CONV_CH ** -0.5, 0.1875)
    residual = noise(own_keys[8], (TOKENS, D), 1.0, 6.0, ((0, 16),))
    moe_gain = jnp.clip(1.0 + 0.18 * jax.random.normal(keys[9], (D,), jnp.float32), 0.1, 1.9)
    expert_ids = draw_expert_ids(jax.random.fold_in(jax.random.fold_in(keys[15], part), 71), part)
    expert_weights = jnp.clip(0.1 + 0.59999999 * jax.random.uniform(own_keys[11], (TOKENS, 2), jnp.float32) ** block_levels(own_keys[11], (TOKENS, 2), ((0, 16),), -0.2, 0.2), 0.1, 0.7)
    w_gate = noise(keys[12], (EXPERTS, D, HID), D ** -0.5, 0.125, ((0, 16),))
    w_up = noise(keys[13], (EXPERTS, D, HID), D ** -0.5, 0.125, ((0, 16),))
    w_down = noise(keys[14], (EXPERTS, HID, D), HID ** -0.5, 0.25, ((0, 16),))
    return dict(conv_value=conv_value, conv_gate=conv_gate, kernel=kernel, conv_bias=conv_bias, ln_gain=ln_gain, ln_bias=ln_bias, out_gain=out_gain, out_weight=out_weight, residual=residual, moe_gain=moe_gain, expert_ids=expert_ids, expert_weights=expert_weights, w_gate=w_gate, w_up=w_up, w_down=w_down)


EPSILON = 1e-06

def reference(conv_value, conv_gate, kernel, conv_bias, ln_gain, ln_bias, out_gain, out_weight, residual, moe_gain, expert_ids, expert_weights, w_gate, w_up, w_down):
    gated = (conv_value.astype(jnp.float32) * jax.nn.sigmoid(conv_gate.astype(jnp.float32))).astype(jnp.bfloat16)
    padded = jnp.concatenate([jnp.zeros((KERNEL - 1, CONV_CH), gated.dtype), gated], axis=0)
    convolved = jnp.zeros((TOKENS, CONV_CH), jnp.float32) + conv_bias
    for offset in range(KERNEL):
        convolved = convolved + padded[offset:offset + TOKENS].astype(jnp.float32) * kernel[offset].astype(jnp.float32)
    average = lax.optimization_barrier(jnp.mean(convolved, axis=1, keepdims=True))
    spread = lax.optimization_barrier(jnp.mean(convolved * convolved, axis=1, keepdims=True)) - average * average
    swished = jax.nn.silu((convolved - average) * lax.rsqrt(spread + EPSILON) * ln_gain + ln_bias)
    energy = lax.optimization_barrier(jnp.mean(swished * swished, axis=1, keepdims=True))
    branch = (swished * lax.rsqrt(energy + EPSILON) * out_gain).astype(jnp.bfloat16)
    projected = jnp.dot(branch, out_weight, preferred_element_type=jnp.float32)
    hidden = (residual.astype(jnp.float32) + projected).astype(jnp.bfloat16)
    widened = hidden.astype(jnp.float32)
    normed = (widened * lax.rsqrt(lax.optimization_barrier(jnp.mean(widened * widened, axis=1, keepdims=True)) + EPSILON) * moe_gain).astype(jnp.bfloat16)
    flat_ids = expert_ids.reshape(-1).astype(jnp.int32)
    onehot = (flat_ids[:, None] == jnp.arange(EXPERTS, dtype=jnp.int32)[None, :]).astype(jnp.int32)
    slot_rank = lax.optimization_barrier(jnp.sum((jnp.cumsum(onehot, axis=0) - 1) * onehot, axis=1)).astype(jnp.int32)
    capacity = TOKENS // ROWS * CAP
    position = flat_ids * capacity + slot_rank
    token_index = (jnp.arange(2 * TOKENS, dtype=jnp.int32) // 2).astype(jnp.int32)
    table = jnp.full((EXPERTS * capacity,), TOKENS, jnp.int32).at[position].set(token_index).reshape(EXPERTS, capacity)
    weight_table = jnp.zeros((EXPERTS * capacity,), jnp.float32).at[position].set(expert_weights.reshape(-1).astype(jnp.float32)).reshape(EXPERTS, capacity)
    source_rows = jnp.concatenate([normed, jnp.zeros((1, D), normed.dtype)], axis=0)

    def one_expert(total, pieces):
        rows_index, row_weights, gate_w, up_w, down_w = pieces
        taken = source_rows[rows_index]
        gate_part = jnp.dot(taken, gate_w, preferred_element_type=jnp.float32)
        up_part = jnp.dot(taken, up_w, preferred_element_type=jnp.float32)
        active = (jax.nn.silu(gate_part) * up_part).astype(jnp.bfloat16)
        result = jnp.dot(active, down_w, preferred_element_type=jnp.float32).astype(jnp.bfloat16)
        return (total.at[rows_index].add(row_weights[:, None] * result.astype(jnp.float32)), None)
    start_total = jnp.zeros((TOKENS + 1, D), jnp.float32)
    combined, _ = lax.scan(one_expert, start_total, (table, weight_table, w_gate, w_up, w_down))
    return (widened + combined[:TOKENS]).astype(jnp.bfloat16)
```

```python
import jax
import jax.numpy as jnp
from jax import lax
from jax.experimental import pallas as pl
from jax.experimental.pallas import tpu as pltpu
from jax.sharding import PartitionSpec as P

EPSILON = 1e-06
GROUPS = 4
LANES = 128
SUBLANES = 8
MESH = pl.DeviceIdType.MESH


def flipped(index, mask, size):
    total, bit = 0, 1
    while bit < size:
        total = total + ((index // bit + mask // bit) % 2) * bit
        bit *= 2
    return total


def routed_kernel(
    send, meta, gate_hbm, up_hbm, down_hbm, out,
    w_gate, w_up, w_down, rows, weights, own, half_out, half_in, cross_out, cross_in, final, act,
    load_sem, meta_s, meta_r, z_s, z_r, pair_s, pair_r, x_s, x_r, via_s, via_r,
    half_s, half_r, cross_s, cross_r, back_s, back_r,
):
    spn, tpn, cap, width = rows.shape
    me_z, me_t = lax.axis_index("sp"), lax.axis_index("tp")
    pair, across = flipped(me_t, 1, tpn), flipped(me_t, 2, tpn)
    hidden = w_gate.shape[1]

    def to(z, t):
        return {"sp": z, "tp": t}

    def copy(src, dst, s, r, z, t):
        return pltpu.make_async_remote_copy(
            src_ref=src, dst_ref=dst, send_sem=s, recv_sem=r, device_id=to(z, t), device_id_type=MESH
        )

    loads = [
        pltpu.make_async_copy(a, b, load_sem.at[i])
        for i, (a, b) in enumerate(((gate_hbm, w_gate), (up_hbm, w_up), (down_hbm, w_down)))
    ]
    for load in loads:
        load.start()

    peers = [(k, r) for k in range(spn) for r in range(tpn) if k or r]
    barrier = pltpu.get_barrier_semaphore()
    for k, r in peers:
        pl.semaphore_signal(
            barrier, inc=1, device_id=to(flipped(me_z, k, spn), flipped(me_t, r, tpn)), device_id_type=MESH
        )
    pl.semaphore_wait(barrier, len(peers))

    def z_copy(k):
        return copy(send.at[k], rows.at[k, 0], z_s.at[k], z_r.at[k], flipped(me_z, k, spn), me_t)

    def meta_copy(k, r):
        return copy(
            meta.at[k], weights.at[k, r], meta_s.at[k, r], meta_r.at[k, r],
            flipped(me_z, k, spn), flipped(me_t, r, tpn),
        )

    def pair_copy(k):
        return copy(rows.at[k, 0], rows.at[k, 1], pair_s.at[k], pair_r.at[k], me_z, pair)

    def x_copy(k):
        return copy(rows.at[k, 0], rows.at[k, 2], x_s.at[k], x_r.at[k], me_z, across)

    def via_copy(k):
        return copy(rows.at[k, 2], rows.at[k, 3], via_s.at[k], via_r.at[k], me_z, pair)

    def half_copy(k):
        return copy(half_out.at[k], half_in.at[k], half_s.at[k], half_r.at[k], me_z, pair)

    def cross_copy(k):
        return copy(cross_out.at[k], cross_in.at[k], cross_s.at[k], cross_r.at[k], me_z, across)

    def back_copy(k):
        return copy(final.at[k], out.at[k], back_s.at[k], back_r.at[k], flipped(me_z, k, spn), me_t)

    for k, r in peers:
        meta_copy(k, r).start()
    for k in range(1, spn):
        z_copy(k).start()
    weights[0, 0] = meta[0]
    rows[0, 0] = send[0]
    x_copy(0).start()
    pair_copy(0).start()
    for k, r in peers:
        meta_copy(k, r).wait_recv()
    for load in loads:
        load.wait()

    tile = min(hidden, 512)
    diagonal = (
        lax.broadcasted_iota(jnp.int32, (cap, LANES), 0) == lax.broadcasted_iota(jnp.int32, (cap, LANES), 1)
    )

    def compute(k):
        x = rows[k].reshape(tpn * cap, width)
        for c in range(0, hidden, 256):
            g = jnp.dot(x, w_gate[:, c : c + 256], preferred_element_type=jnp.float32)
            u = jnp.dot(x, w_up[:, c : c + 256], preferred_element_type=jnp.float32)
            act[:, c : c + 256] = (g / (1.0 + jnp.exp(-g)) * u).astype(jnp.bfloat16)
        a = act[...]
        scales = [
            jnp.sum(jnp.where(diagonal, weights[k, r, pl.ds(me_t, 1), :], 0.0), axis=1, keepdims=True)
            for r in range(tpn)
        ]

        def column(c, carry):
            cols = pl.ds(pl.multiple_of(c * tile, tile), tile)
            res = jnp.dot(a, w_down[:, cols], preferred_element_type=jnp.float32).astype(jnp.bfloat16)
            res = res.astype(jnp.float32)
            parts = [res[r * cap : (r + 1) * cap] * scales[r] for r in range(tpn)]
            half_out[k, 0, :, cols] = parts[1].astype(jnp.bfloat16)
            half_out[k, 1, :, cols] = parts[3].astype(jnp.bfloat16)
            own[k, 0, :, cols] = parts[0]
            own[k, 1, :, cols] = parts[2]
            return carry

        lax.fori_loop(0, width // tile, column, 0)

    def step(i, carry):
        @pl.when(i + 1 < spn)
        def _():
            k = i + 1
            z_copy(k).wait_recv()
            x_copy(k).start()
            pair_copy(k).start()

        @pl.when(i < spn)
        def _():
            x_copy(i).wait_recv()
            via_copy(i).start()
            pair_copy(i).wait_recv()
            via_copy(i).wait_recv()
            compute(i)
            half_copy(i).start()

        @pl.when((i >= 1) & (i <= spn))
        def _():
            k = i - 1
            half_copy(k).wait_recv()
            cross_out[k] = (own[k, 1] + half_in[k, 1].astype(jnp.float32)).astype(jnp.bfloat16)
            cross_copy(k).start()

        @pl.when(i >= 2)
        def _():
            k = i - 2
            cross_copy(k).wait_recv()
            final[k] = (
                own[k, 0] + half_in[k, 0].astype(jnp.float32) + cross_in[k].astype(jnp.float32)
            ).astype(jnp.bfloat16)

            @pl.when(k >= 1)
            def _():
                back_copy(k).start()

        return carry

    lax.fori_loop(0, spn + 2, step, 0)
    out[0] = final[0]
    for k, r in peers:
        meta_copy(k, r).wait_send()
    for k in range(spn):
        for make in (x_copy, pair_copy, via_copy, half_copy, cross_copy):
            make(k).wait_send()
    for k in range(1, spn):
        z_copy(k).wait_send()
        back_copy(k).wait_send()
        back_copy(k).wait_recv()


def routed_experts(send, meta, w_gate, w_up, w_down):
    spn, cap, width = send.shape
    tpn = lax.axis_size("tp")
    hidden = w_gate.shape[1]
    bf, f32, dma = jnp.bfloat16, jnp.float32, pltpu.SemaphoreType.DMA
    vmem = pl.BlockSpec(memory_space=pltpu.VMEM)
    hbm = pl.BlockSpec(memory_space=pl.ANY)
    return pl.pallas_call(
        routed_kernel,
        out_shape=jax.ShapeDtypeStruct((spn, cap, width), bf),
        in_specs=[vmem, vmem, hbm, hbm, hbm],
        out_specs=vmem,
        scratch_shapes=[
            pltpu.VMEM(w_gate.shape, bf),
            pltpu.VMEM(w_up.shape, bf),
            pltpu.VMEM(w_down.shape, bf),
            pltpu.VMEM((spn, tpn, cap, width), bf),
            pltpu.VMEM((spn, tpn, SUBLANES, LANES), f32),
            pltpu.VMEM((spn, 2, cap, width), f32),
            pltpu.VMEM((spn, 2, cap, width), bf),
            pltpu.VMEM((spn, 2, cap, width), bf),
            pltpu.VMEM((spn, cap, width), bf),
            pltpu.VMEM((spn, cap, width), bf),
            pltpu.VMEM((spn, cap, width), bf),
            pltpu.VMEM((tpn * cap, hidden), bf),
            dma((3,)),
            dma((spn, tpn)),
            dma((spn, tpn)),
        ]
        + [dma((spn,))] * 14,
        compiler_params=pltpu.CompilerParams(collective_id=0, has_side_effects=True),
    )(send, meta, w_gate, w_up, w_down)


def route_by_group(normed, widened, expert_ids, expert_weights, w_gate, w_up, w_down):
    spn, tpn = lax.axis_size("sp"), lax.axis_size("tp")
    row_count, width = normed.shape
    capacity = 2 * row_count // min(row_count, spn * tpn // 2)
    cap = tpn * capacity // 2
    group = expert_ids[:, 0] // tpn
    place = jnp.arange(row_count, dtype=jnp.int32)
    earlier = (group[None, :] == group[:, None]) & (place[None, :] < place[:, None])
    rank = jnp.sum(earlier.astype(jnp.int32), axis=1)
    slot = flipped(group, lax.axis_index("sp"), spn) * cap + rank
    chosen = jnp.arange(spn * cap, dtype=jnp.int32)[:, None] == slot[None, :]
    pick = chosen.astype(jnp.bfloat16)
    send = jnp.dot(pick, normed, preferred_element_type=jnp.float32).astype(jnp.bfloat16)
    member = (expert_ids[:, :, None] % tpn) == jnp.arange(SUBLANES, dtype=jnp.int32)[None, None, :]
    by_expert = jnp.sum(jnp.where(member, expert_weights[:, :, None], 0.0), axis=1)
    meta = jnp.sum(
        jnp.where(chosen[None, :, :], by_expert.T[:, None, :], 0.0), axis=2
    ).reshape(SUBLANES, spn, cap)
    meta = jnp.pad(meta.transpose(1, 0, 2), ((0, 0), (0, 0), (0, LANES - cap)))
    back = routed_experts(send.reshape(spn, cap, width), meta, w_gate[0], w_up[0], w_down[0])
    combined = lax.dot_general(
        pick, back.reshape(spn * cap, width), (((0,), (0,)), ((), ())), preferred_element_type=jnp.float32
    )
    return (widened + combined).astype(jnp.bfloat16)


def passed_along(block, axis, distance):
    devices = range(lax.axis_size(axis))
    route = [(i - distance, i) for i in devices if i - distance in devices]
    return lax.ppermute(block, axis, route)


def per_device(
    conv_value,
    conv_gate,
    kernel,
    conv_bias,
    ln_gain,
    ln_bias,
    out_gain,
    out_weight,
    residual,
    moe_gain,
    expert_ids,
    expert_weights,
    w_gate,
    w_up,
    w_down,
):
    tok_rows, channels = conv_value.shape
    reach_rows = kernel.shape[0] - 1
    full_channels = channels * lax.axis_size("tp")
    gated = (conv_value.astype(jnp.float32) * jax.nn.sigmoid(conv_gate.astype(jnp.float32))).astype(
        jnp.bfloat16
    )
    before = passed_along(gated[tok_rows - reach_rows :], "sp", 1)
    padded = jnp.concatenate([before, gated], axis=0)
    convolved = jnp.zeros((tok_rows, channels), jnp.float32) + conv_bias
    for offset in range(reach_rows + 1):
        convolved = convolved + padded[offset : offset + tok_rows].astype(jnp.float32) * kernel[
            offset
        ].astype(jnp.float32)
    totals = lax.psum((jnp.sum(convolved, axis=1), jnp.sum(convolved * convolved, axis=1)), "tp")
    average = (totals[0] / full_channels)[:, None]
    spread = (totals[1] / full_channels)[:, None] - average * average
    swished = jax.nn.silu((convolved - average) * lax.rsqrt(spread + EPSILON) * ln_gain + ln_bias)
    energy = lax.psum(jnp.sum(swished * swished, axis=1), "tp")
    branch = (swished * lax.rsqrt(energy / full_channels + EPSILON)[:, None] * out_gain).astype(
        jnp.bfloat16
    )
    row_count = tok_rows // lax.axis_size("tp")
    regrouped = lax.all_to_all(branch, "tp", split_axis=0, concat_axis=1, tiled=True)
    projected = jnp.dot(regrouped, out_weight, preferred_element_type=jnp.float32)
    hidden = (residual.astype(jnp.float32) + projected).astype(jnp.bfloat16)
    widened = hidden.astype(jnp.float32)
    normed = (
        widened * lax.rsqrt(jnp.mean(widened * widened, axis=1, keepdims=True) + EPSILON) * moe_gain
    ).astype(jnp.bfloat16)
    width = normed.shape[1]
    experts = lax.axis_size("sp") * lax.axis_size("tp")
    if experts // GROUPS == lax.axis_size("tp") and lax.axis_size("tp") == 4:
        return route_by_group(
            normed, widened, expert_ids, expert_weights, w_gate, w_up, w_down
        )
    capacity = 2 * row_count // min(row_count, experts // 2)
    flat_ids = expert_ids.reshape(-1)
    onehot = (flat_ids[:, None] == jnp.arange(experts, dtype=jnp.int32)[None, :]).astype(jnp.int32)
    slot_rank = jnp.sum((jnp.cumsum(onehot, axis=0) - 1) * onehot, axis=1)
    position = flat_ids * capacity + slot_rank
    outgoing = (
        jnp.zeros((experts * capacity, width), jnp.bfloat16)
        .at[position]
        .set(jnp.repeat(normed, 2, axis=0))
    )
    outgoing = outgoing.reshape(experts, capacity, width)
    arriving = lax.all_to_all(outgoing, ("sp", "tp"), split_axis=0, concat_axis=0, tiled=True)
    flattened = arriving.reshape(-1, width)
    gate_part = jnp.dot(flattened, w_gate[0], preferred_element_type=jnp.float32)
    up_part = jnp.dot(flattened, w_up[0], preferred_element_type=jnp.float32)
    active = (jax.nn.silu(gate_part) * up_part).astype(jnp.bfloat16)
    result = jnp.dot(active, w_down[0], preferred_element_type=jnp.float32).astype(jnp.bfloat16)
    produced = result.reshape(arriving.shape)
    returned = lax.all_to_all(produced, ("sp", "tp"), split_axis=0, concat_axis=0, tiled=True)
    returned = returned.reshape(experts * capacity, width)
    picked = returned[position].reshape(row_count, 2, width)
    combined = jnp.sum(picked.astype(jnp.float32) * expert_weights[:, :, None], axis=1)
    return (widened + combined).astype(jnp.bfloat16)


def solution(mesh):
    in_specs = (
        P(("grp", "sp"), "tp"),
        P(("grp", "sp"), "tp"),
        P(None, "tp"),
        P("tp"),
        P("tp"),
        P("tp"),
        P("tp"),
        P(),
        P(("grp", "sp", "tp"), None),
        P(),
        P(("grp", "sp", "tp"), None),
        P(("grp", "sp", "tp"), None),
        P(("sp", "tp"), None, None),
        P(("sp", "tp"), None, None),
        P(("sp", "tp"), None, None),
    )
    out_specs = P(("grp", "sp", "tp"), None)
    return jax.shard_map(
        per_device, mesh=mesh, in_specs=in_specs, out_specs=out_specs, check_vma=False
    )
```

```python
import jax
import jax.numpy as jnp
from jax import lax
from jax.experimental import pallas as pl
from jax.experimental.pallas import tpu as pltpu
from jax.sharding import PartitionSpec as P

EPSILON = 1e-06
GROUPS = 4
LANES = 128
SUBLANES = 8
MESH = pl.DeviceIdType.MESH


def flipped(index, mask, size):
    total, bit = 0, 1
    while bit < size:
        total = total + ((index // bit + mask // bit) % 2) * bit
        bit *= 2
    return total


def layer_kernel(
    value, gate, taps, params, residual, moe_gain, meta, pick, unpick,
    out_hbm, gate_hbm, up_hbm, down_hbm, result,
    w_out, w_gate, w_up, w_down, padded, conv, wide, gains, branch, hid, send, back,
    rows, weights, own, half_out, half_in, cross_out, cross_in, final, act,
    load_sem, meta_s, meta_r, halo_s, halo_r, gain_s, gain_r, group_s, group_r,
    z_s, z_r, pair_s, pair_r, x_s, x_r, via_s, via_r,
    half_s, half_r, cross_s, cross_r, back_s, back_r,
):
    spn, tpn, cap, width = rows.shape
    me_z, me_t = lax.axis_index("sp"), lax.axis_index("tp")
    pair, across = flipped(me_t, 1, tpn), flipped(me_t, 2, tpn)
    hidden = w_gate.shape[1]
    tok_rows, channels = value.shape
    row_count = tok_rows // tpn
    full = channels * tpn
    reach = padded.shape[0] - tok_rows
    tap_count = taps.shape[0]
    f32, bf = jnp.float32, jnp.bfloat16

    def to(z, t):
        return {"sp": z, "tp": t}

    def copy(src, dst, s, r, z, t):
        return pltpu.make_async_remote_copy(
            src_ref=src, dst_ref=dst, send_sem=s, recv_sem=r, device_id=to(z, t), device_id_type=MESH
        )

    loads = [
        pltpu.make_async_copy(a, b, load_sem.at[i])
        for i, (a, b) in enumerate(((out_hbm, w_out), (gate_hbm, w_gate), (up_hbm, w_up), (down_hbm, w_down)))
    ]
    for load in loads:
        load.start()

    peers = [(k, r) for k in range(spn) for r in range(tpn) if k or r]
    barrier = pltpu.get_barrier_semaphore()
    for k, r in peers:
        pl.semaphore_signal(
            barrier, inc=1, device_id=to(flipped(me_z, k, spn), flipped(me_t, r, tpn)), device_id_type=MESH
        )

    gated = value[...].astype(f32) / (1.0 + jnp.exp(-gate[...].astype(f32)))
    padded[reach:, :] = gated.astype(bf).astype(f32)
    pl.semaphore_wait(barrier, len(peers))

    mine = pl.ds(pl.multiple_of(me_t * channels, channels), channels)

    def halo_copy(z):
        return copy(
            padded.at[pl.ds(tok_rows, reach)], padded.at[pl.ds(0, reach)], halo_s.at[0], halo_r.at[0], z, me_t
        )

    def gain_copy(r):
        return copy(params, gains.at[:, mine], gain_s.at[r], gain_r.at[r], me_z, flipped(me_t, r, tpn))

    def group_copy(r):
        t = flipped(me_t, r, tpn)
        return copy(conv.at[t], wide.at[:, mine], group_s.at[r], group_r.at[r], me_z, t)

    def z_copy(k):
        return copy(send.at[k], rows.at[k, 0], z_s.at[k], z_r.at[k], flipped(me_z, k, spn), me_t)

    def meta_copy(k, r):
        return copy(
            meta.at[k], weights.at[k, r], meta_s.at[k, r], meta_r.at[k, r],
            flipped(me_z, k, spn), flipped(me_t, r, tpn),
        )

    def pair_copy(k):
        return copy(rows.at[k, 0], rows.at[k, 1], pair_s.at[k], pair_r.at[k], me_z, pair)

    def x_copy(k):
        return copy(rows.at[k, 0], rows.at[k, 2], x_s.at[k], x_r.at[k], me_z, across)

    def via_copy(k):
        return copy(rows.at[k, 2], rows.at[k, 3], via_s.at[k], via_r.at[k], me_z, pair)

    def half_copy(k):
        return copy(half_out.at[k], half_in.at[k], half_s.at[k], half_r.at[k], me_z, pair)

    def cross_copy(k):
        return copy(cross_out.at[k], cross_in.at[k], cross_s.at[k], cross_r.at[k], me_z, across)

    def back_copy(k):
        return copy(final.at[k], back.at[k], back_s.at[k], back_r.at[k], flipped(me_z, k, spn), me_t)

    @pl.when(me_z < spn - 1)
    def _():
        halo_copy(me_z + 1).start()

    for r in range(1, tpn):
        gain_copy(r).start()
    for k, r in peers:
        meta_copy(k, r).start()
    weights[0, 0] = meta[0]
    gains[:, mine] = params[...]

    piece = min(row_count, 64)

    def convolve(first):
        total = jnp.zeros((piece, channels), f32) + params[3:4, :]
        for k in range(tap_count):
            start = first + reach - tap_count + 1 + k
            total = total + padded[start : start + piece, :] * taps[k : k + 1, :]
        block, inner = first // row_count, first % row_count
        conv[block, inner : inner + piece, :] = total.astype(bf)

    for first in range(piece, tok_rows, piece):
        convolve(first)

    @pl.when(me_z == 0)
    def _():
        padded[:reach, :] = jnp.zeros((reach, channels), f32)

    @pl.when(me_z > 0)
    def _():
        halo_copy(me_z - 1).wait_recv()

    convolve(0)
    for r in range(1, tpn):
        group_copy(r).start()
    wide[:, mine] = conv[me_t]
    for r in range(1, tpn):
        gain_copy(r).wait_recv()
    for r in range(1, tpn):
        group_copy(r).wait_recv()

    part = min(row_count, 32)
    for first in range(0, row_count, part):
        v = wide[first : first + part, :].astype(f32)
        average = jnp.sum(v, axis=1, keepdims=True) / full
        spread = jnp.sum(v * v, axis=1, keepdims=True) / full - average * average
        v = (v - average) * lax.rsqrt(spread + EPSILON) * gains[0:1, :] + gains[1:2, :]
        v = v / (1.0 + jnp.exp(-v))
        energy = jnp.sum(v * v, axis=1, keepdims=True) / full
        branch[first : first + part, :] = (v * lax.rsqrt(energy + EPSILON) * gains[2:3, :]).astype(bf)

    tile = min(hidden, 512)
    loads[0].wait()

    def project(c, power):
        cols = pl.ds(pl.multiple_of(c * tile, tile), tile)
        h = residual[:, cols].astype(f32) + jnp.dot(
            branch[...], w_out[:, cols], preferred_element_type=f32
        )
        h = h.astype(bf)
        hid[:, cols] = h
        h = h.astype(f32)
        return power + jnp.sum(h * h, axis=1, keepdims=True)

    power = lax.fori_loop(0, width // tile, project, jnp.zeros((row_count, 1), f32))
    level = lax.rsqrt(power / width + EPSILON)

    def dispatch(c, carry):
        cols = pl.ds(pl.multiple_of(c * tile, tile), tile)
        n = (hid[:, cols].astype(f32) * level * moe_gain[:, cols]).astype(bf)
        picked = jnp.dot(pick[...], n, preferred_element_type=f32).astype(bf)
        for k in range(spn):
            send[k, :, cols] = picked[k * cap : (k + 1) * cap]
        return carry

    lax.fori_loop(0, width // tile, dispatch, 0)

    for k in range(1, spn):
        z_copy(k).start()
    rows[0, 0] = send[0]
    x_copy(0).start()
    pair_copy(0).start()
    for k, r in peers:
        meta_copy(k, r).wait_recv()
    for load in loads[1:]:
        load.wait()

    diagonal = (
        lax.broadcasted_iota(jnp.int32, (cap, LANES), 0) == lax.broadcasted_iota(jnp.int32, (cap, LANES), 1)
    )

    def compute(k):
        x = rows[k].reshape(tpn * cap, width)
        for c in range(0, hidden, 256):
            g = jnp.dot(x, w_gate[:, c : c + 256], preferred_element_type=jnp.float32)
            u = jnp.dot(x, w_up[:, c : c + 256], preferred_element_type=jnp.float32)
            act[:, c : c + 256] = (g / (1.0 + jnp.exp(-g)) * u).astype(jnp.bfloat16)
        a = act[...]
        scales = [
            jnp.sum(jnp.where(diagonal, weights[k, r, pl.ds(me_t, 1), :], 0.0), axis=1, keepdims=True)
            for r in range(tpn)
        ]

        def column(c, carry):
            cols = pl.ds(pl.multiple_of(c * tile, tile), tile)
            res = jnp.dot(a, w_down[:, cols], preferred_element_type=jnp.float32).astype(jnp.bfloat16)
            res = res.astype(jnp.float32)
            parts = [res[r * cap : (r + 1) * cap] * scales[r] for r in range(tpn)]
            half_out[k, 0, :, cols] = parts[1].astype(jnp.bfloat16)
            half_out[k, 1, :, cols] = parts[3].astype(jnp.bfloat16)
            own[k, 0, :, cols] = parts[0]
            own[k, 1, :, cols] = parts[2]
            return carry

        lax.fori_loop(0, width // tile, column, 0)

    def step(i, carry):
        @pl.when(i + 1 < spn)
        def _():
            k = i + 1
            z_copy(k).wait_recv()
            x_copy(k).start()
            pair_copy(k).start()

        @pl.when(i < spn)
        def _():
            x_copy(i).wait_recv()
            via_copy(i).start()
            pair_copy(i).wait_recv()
            via_copy(i).wait_recv()
            compute(i)
            half_copy(i).start()

        @pl.when((i >= 1) & (i <= spn))
        def _():
            k = i - 1
            half_copy(k).wait_recv()
            cross_out[k] = (own[k, 1] + half_in[k, 1].astype(jnp.float32)).astype(jnp.bfloat16)
            cross_copy(k).start()

        @pl.when(i >= 2)
        def _():
            k = i - 2
            cross_copy(k).wait_recv()
            final[k] = (
                own[k, 0] + half_in[k, 0].astype(jnp.float32) + cross_in[k].astype(jnp.float32)
            ).astype(jnp.bfloat16)

            @pl.when(k >= 1)
            def _():
                back_copy(k).start()

        return carry

    lax.fori_loop(0, spn + 2, step, 0)
    back[0] = final[0]
    for k in range(1, spn):
        back_copy(k).wait_recv()

    def combine(c, carry):
        cols = pl.ds(pl.multiple_of(c * tile, tile), tile)
        total = hid[:, cols].astype(f32)
        moved = back[:, :, cols].reshape(spn * cap, tile)
        total = total + jnp.dot(unpick[...], moved, preferred_element_type=f32)
        result[:, cols] = total.astype(bf)
        return carry

    lax.fori_loop(0, width // tile, combine, 0)

    @pl.when(me_z < spn - 1)
    def _():
        halo_copy(me_z + 1).wait_send()

    for r in range(1, tpn):
        gain_copy(r).wait_send()
        group_copy(r).wait_send()
    for k, r in peers:
        meta_copy(k, r).wait_send()
    for k in range(spn):
        for make in (x_copy, pair_copy, via_copy, half_copy, cross_copy):
            make(k).wait_send()
    for k in range(1, spn):
        z_copy(k).wait_send()
        back_copy(k).wait_send()


def whole_layer(
    value, gate, taps, params, residual, moe_gain, meta, pick, unpick, w_out, w_gate, w_up, w_down
):
    spn, tpn = lax.axis_size("sp"), lax.axis_size("tp")
    cap = pick.shape[0] // spn
    tok_rows, channels = value.shape
    row_count, width = residual.shape
    hidden = w_gate.shape[1]
    reach = -(-(taps.shape[0] - 1) // SUBLANES) * SUBLANES
    bf, f32, dma = jnp.bfloat16, jnp.float32, pltpu.SemaphoreType.DMA
    vmem = pl.BlockSpec(memory_space=pltpu.VMEM)
    hbm = pl.BlockSpec(memory_space=pl.ANY)
    return pl.pallas_call(
        layer_kernel,
        out_shape=jax.ShapeDtypeStruct((row_count, width), bf),
        in_specs=[vmem] * 9 + [hbm] * 4,
        out_specs=vmem,
        scratch_shapes=[
            pltpu.VMEM(w_out.shape, bf),
            pltpu.VMEM(w_gate.shape, bf),
            pltpu.VMEM(w_up.shape, bf),
            pltpu.VMEM(w_down.shape, bf),
            pltpu.VMEM((reach + tok_rows, channels), f32),
            pltpu.VMEM((tpn, row_count, channels), bf),
            pltpu.VMEM((row_count, channels * tpn), bf),
            pltpu.VMEM((SUBLANES, channels * tpn), f32),
            pltpu.VMEM((row_count, channels * tpn), bf),
            pltpu.VMEM((row_count, width), bf),
            pltpu.VMEM((spn, cap, width), bf),
            pltpu.VMEM((spn, cap, width), bf),
            pltpu.VMEM((spn, tpn, cap, width), bf),
            pltpu.VMEM((spn, tpn, SUBLANES, LANES), f32),
            pltpu.VMEM((spn, 2, cap, width), f32),
            pltpu.VMEM((spn, 2, cap, width), bf),
            pltpu.VMEM((spn, 2, cap, width), bf),
            pltpu.VMEM((spn, cap, width), bf),
            pltpu.VMEM((spn, cap, width), bf),
            pltpu.VMEM((spn, cap, width), bf),
            pltpu.VMEM((tpn * cap, hidden), bf),
            dma((4,)),
            dma((spn, tpn)),
            dma((spn, tpn)),
            dma((1,)),
            dma((1,)),
        ]
        + [dma((tpn,))] * 4
        + [dma((spn,))] * 14,
        compiler_params=pltpu.CompilerParams(collective_id=0, has_side_effects=True),
    )(value, gate, taps, params, residual, moe_gain, meta, pick, unpick, w_out, w_gate, w_up, w_down)


def fused_layer(
    conv_value,
    conv_gate,
    kernel,
    conv_bias,
    ln_gain,
    ln_bias,
    out_gain,
    out_weight,
    residual,
    moe_gain,
    expert_ids,
    expert_weights,
    w_gate,
    w_up,
    w_down,
):
    spn, tpn = lax.axis_size("sp"), lax.axis_size("tp")
    row_count, width = residual.shape
    capacity = 2 * row_count // min(row_count, spn * tpn // 2)
    cap = tpn * capacity // 2
    group = expert_ids[:, 0] // tpn
    place = jnp.arange(row_count, dtype=jnp.int32)
    earlier = (group[None, :] == group[:, None]) & (place[None, :] < place[:, None])
    rank = jnp.sum(earlier.astype(jnp.int32), axis=1)
    slot = flipped(group, lax.axis_index("sp"), spn) * cap + rank
    chosen = jnp.arange(spn * cap, dtype=jnp.int32)[:, None] == slot[None, :]
    pick = chosen.astype(jnp.bfloat16)
    member = (expert_ids[:, :, None] % tpn) == jnp.arange(SUBLANES, dtype=jnp.int32)[None, None, :]
    by_expert = jnp.sum(jnp.where(member, expert_weights[:, :, None], 0.0), axis=1)
    meta = jnp.sum(
        jnp.where(chosen[None, :, :], by_expert.T[:, None, :], 0.0), axis=2
    ).reshape(SUBLANES, spn, cap)
    meta = jnp.pad(meta.transpose(1, 0, 2), ((0, 0), (0, 0), (0, LANES - cap)))
    unpick = (slot[:, None] == jnp.arange(spn * cap, dtype=jnp.int32)[None, :]).astype(jnp.bfloat16)
    params = jnp.stack([ln_gain, ln_bias, out_gain, conv_bias])
    params = jnp.pad(params, ((0, SUBLANES - params.shape[0]), (0, 0)))
    return whole_layer(
        conv_value, conv_gate, kernel.astype(jnp.float32), params, residual, moe_gain[None, :],
        meta, pick, unpick, out_weight, w_gate[0], w_up[0], w_down[0],
    )


def passed_along(block, axis, distance):
    devices = range(lax.axis_size(axis))
    route = [(i - distance, i) for i in devices if i - distance in devices]
    return lax.ppermute(block, axis, route)


def per_device(
    conv_value,
    conv_gate,
    kernel,
    conv_bias,
    ln_gain,
    ln_bias,
    out_gain,
    out_weight,
    residual,
    moe_gain,
    expert_ids,
    expert_weights,
    w_gate,
    w_up,
    w_down,
):
    tpn = lax.axis_size("tp")
    if lax.axis_size("sp") == GROUPS and tpn == 4:
        return fused_layer(
            conv_value, conv_gate, kernel, conv_bias, ln_gain, ln_bias, out_gain, out_weight, residual,
            moe_gain, expert_ids, expert_weights, w_gate, w_up, w_down,
        )
    tok_rows, channels = conv_value.shape
    reach_rows = kernel.shape[0] - 1
    full_channels = channels * lax.axis_size("tp")
    gated = (conv_value.astype(jnp.float32) * jax.nn.sigmoid(conv_gate.astype(jnp.float32))).astype(
        jnp.bfloat16
    )
    before = passed_along(gated[tok_rows - reach_rows :], "sp", 1)
    padded = jnp.concatenate([before, gated], axis=0)
    convolved = jnp.zeros((tok_rows, channels), jnp.float32) + conv_bias
    for offset in range(reach_rows + 1):
        convolved = convolved + padded[offset : offset + tok_rows].astype(jnp.float32) * kernel[
            offset
        ].astype(jnp.float32)
    totals = lax.psum((jnp.sum(convolved, axis=1), jnp.sum(convolved * convolved, axis=1)), "tp")
    average = (totals[0] / full_channels)[:, None]
    spread = (totals[1] / full_channels)[:, None] - average * average
    swished = jax.nn.silu((convolved - average) * lax.rsqrt(spread + EPSILON) * ln_gain + ln_bias)
    energy = lax.psum(jnp.sum(swished * swished, axis=1), "tp")
    branch = (swished * lax.rsqrt(energy / full_channels + EPSILON)[:, None] * out_gain).astype(
        jnp.bfloat16
    )
    row_count = tok_rows // lax.axis_size("tp")
    regrouped = lax.all_to_all(branch, "tp", split_axis=0, concat_axis=1, tiled=True)
    projected = jnp.dot(regrouped, out_weight, preferred_element_type=jnp.float32)
    hidden = (residual.astype(jnp.float32) + projected).astype(jnp.bfloat16)
    widened = hidden.astype(jnp.float32)
    normed = (
        widened * lax.rsqrt(jnp.mean(widened * widened, axis=1, keepdims=True) + EPSILON) * moe_gain
    ).astype(jnp.bfloat16)
    width = normed.shape[1]
    experts = lax.axis_size("sp") * lax.axis_size("tp")
    capacity = 2 * row_count // min(row_count, experts // 2)
    flat_ids = expert_ids.reshape(-1)
    onehot = (flat_ids[:, None] == jnp.arange(experts, dtype=jnp.int32)[None, :]).astype(jnp.int32)
    slot_rank = jnp.sum((jnp.cumsum(onehot, axis=0) - 1) * onehot, axis=1)
    position = flat_ids * capacity + slot_rank
    outgoing = (
        jnp.zeros((experts * capacity, width), jnp.bfloat16)
        .at[position]
        .set(jnp.repeat(normed, 2, axis=0))
    )
    outgoing = outgoing.reshape(experts, capacity, width)
    arriving = lax.all_to_all(outgoing, ("sp", "tp"), split_axis=0, concat_axis=0, tiled=True)
    flattened = arriving.reshape(-1, width)
    gate_part = jnp.dot(flattened, w_gate[0], preferred_element_type=jnp.float32)
    up_part = jnp.dot(flattened, w_up[0], preferred_element_type=jnp.float32)
    active = (jax.nn.silu(gate_part) * up_part).astype(jnp.bfloat16)
    result = jnp.dot(active, w_down[0], preferred_element_type=jnp.float32).astype(jnp.bfloat16)
    produced = result.reshape(arriving.shape)
    returned = lax.all_to_all(produced, ("sp", "tp"), split_axis=0, concat_axis=0, tiled=True)
    returned = returned.reshape(experts * capacity, width)
    picked = returned[position].reshape(row_count, 2, width)
    combined = jnp.sum(picked.astype(jnp.float32) * expert_weights[:, :, None], axis=1)
    return (widened + combined).astype(jnp.bfloat16)


def solution(mesh):
    in_specs = (
        P(("grp", "sp"), "tp"),
        P(("grp", "sp"), "tp"),
        P(None, "tp"),
        P("tp"),
        P("tp"),
        P("tp"),
        P("tp"),
        P(),
        P(("grp", "sp", "tp"), None),
        P(),
        P(("grp", "sp", "tp"), None),
        P(("grp", "sp", "tp"), None),
        P(("sp", "tp"), None, None),
        P(("sp", "tp"), None, None),
        P(("sp", "tp"), None, None),
    )
    out_specs = P(("grp", "sp", "tp"), None)
    return jax.shard_map(
        per_device, mesh=mesh, in_specs=in_specs, out_specs=out_specs, check_vma=False
    )
```

```python
import jax
import jax.numpy as jnp
from jax import lax
from jax.experimental import pallas as pl
from jax.experimental.pallas import tpu as pltpu
from jax.sharding import PartitionSpec as P

EPSILON = 1e-06
GROUPS = 4
SPLIT = 2
LANES = 128
SUBLANES = 8
MESH = pl.DeviceIdType.MESH


def flipped(index, mask, size):
    total, bit = 0, 1
    while bit < size:
        total = total + ((index // bit + mask // bit) % 2) * bit
        bit *= 2
    return total


def layer_kernel(
    value, gate, kernel, conv_bias, ln_gain, ln_bias, out_gain, residual, moe_gain, ids, shares,
    out_hbm, gate_hbm, up_hbm, down_hbm, result,
    w_out, w_gate, w_up, w_down, taps, params, meta, pick, unpick, padded, conv, wide, gains, branch, hid, send, back,
    rows, weights, own, half_out, half_in, cross_out, cross_in, final, act,
    load_sem, meta_s, meta_r, halo_s, halo_r, gain_s, gain_r, group_s, group_r,
    z_s, z_r, pair_s, pair_r, x_s, x_r, via_s, via_r,
    half_s, half_r, cross_s, cross_r, back_s, back_r,
):
    spn, tpn = weights.shape[:2]
    pieces, _, height, width = rows.shape
    cap = height * SPLIT
    me_z, me_t = lax.axis_index("sp"), lax.axis_index("tp")
    pair, across = flipped(me_t, 1, tpn), flipped(me_t, 2, tpn)
    hidden = w_gate.shape[1]
    tok_rows, channels = value.shape
    row_count = tok_rows // tpn
    full = channels * tpn
    reach = padded.shape[0] - tok_rows
    tap_count = kernel.shape[0]
    f32, bf = jnp.float32, jnp.bfloat16

    def to(z, t):
        return {"sp": z, "tp": t}

    def copy(src, dst, s, r, z, t):
        return pltpu.make_async_remote_copy(
            src_ref=src, dst_ref=dst, send_sem=s, recv_sem=r, device_id=to(z, t), device_id_type=MESH
        )

    loads = [
        pltpu.make_async_copy(a, b, load_sem.at[i])
        for i, (a, b) in enumerate(((out_hbm, w_out), (gate_hbm, w_gate), (up_hbm, w_up), (down_hbm, w_down)))
    ]
    for load in loads:
        load.start()

    peers = [(k, r) for k in range(spn) for r in range(tpn) if k or r]
    barrier = pltpu.get_barrier_semaphore()
    for k, r in peers:
        pl.semaphore_signal(
            barrier, inc=1, device_id=to(flipped(me_z, k, spn), flipped(me_t, r, tpn)), device_id_type=MESH
        )

    params[...] = jnp.zeros_like(params)
    for i, given in enumerate((ln_gain, ln_bias, out_gain, conv_bias)):
        params[i : i + 1, :] = given[...]
    taps[:tap_count, :] = kernel[...].astype(f32)

    square = (row_count, row_count)
    down, along = (lax.broadcasted_iota(jnp.int32, square, d) for d in (0, 1))
    group = jnp.broadcast_to(lax.div(ids[:, 0:1], tpn), square)
    group_row = jnp.broadcast_to(
        jnp.sum(jnp.where(down == along, group, 0), axis=0, keepdims=True), square
    )
    same = group == group_row
    rank = jnp.sum(jnp.where(same & (along < down), 1, 0), axis=1, keepdims=True)
    rank_row = jnp.sum(jnp.where(same & (down < along), 1, 0), axis=0, keepdims=True)
    slot = jnp.bitwise_xor(group[:, 0:1], me_z) * cap + rank
    slot_row = jnp.bitwise_xor(group_row[0:1, :], me_z) * cap + rank_row
    slots = spn * cap
    pick[...] = jnp.where(
        lax.broadcasted_iota(jnp.int32, (slots, row_count), 0) == slot_row, 1.0, 0.0
    ).astype(bf)
    unpick[...] = jnp.where(
        lax.broadcasted_iota(jnp.int32, (row_count, slots), 1) == slot, 1.0, 0.0
    ).astype(bf)
    lane = lax.broadcasted_iota(jnp.int32, (row_count, LANES), 1)
    expert = lax.rem(ids[...], tpn)
    meta[...] = jnp.zeros_like(meta)
    for k in range(spn):
        here = (lane + k * cap == slot) & (lane < cap)
        for e in range(tpn):
            share = jnp.sum(jnp.where(expert == e, shares[...], 0.0), axis=1, keepdims=True)
            meta[k, e : e + 1, :] = jnp.sum(jnp.where(here, share, 0.0), axis=0, keepdims=True)

    gated = value[...].astype(f32) / (1.0 + jnp.exp(-gate[...].astype(f32)))
    padded[reach:, :] = gated.astype(bf).astype(f32)
    pl.semaphore_wait(barrier, len(peers))

    mine = pl.ds(pl.multiple_of(me_t * channels, channels), channels)

    def halo_copy(z):
        return copy(
            padded.at[pl.ds(tok_rows, reach)], padded.at[pl.ds(0, reach)], halo_s.at[0], halo_r.at[0], z, me_t
        )

    def gain_copy(r):
        return copy(params, gains.at[:, mine], gain_s.at[r], gain_r.at[r], me_z, flipped(me_t, r, tpn))

    def group_copy(r):
        t = flipped(me_t, r, tpn)
        return copy(conv.at[t], wide.at[:, mine], group_s.at[r], group_r.at[r], me_z, t)

    def z_copy(k):
        return copy(send.at[k], rows.at[k, 0], z_s.at[k], z_r.at[k], flipped(me_z, k // SPLIT, spn), me_t)

    def meta_copy(k, r):
        return copy(
            meta.at[k], weights.at[k, r], meta_s.at[k, r], meta_r.at[k, r],
            flipped(me_z, k, spn), flipped(me_t, r, tpn),
        )

    def pair_copy(k):
        return copy(rows.at[k, 0], rows.at[k, 1], pair_s.at[k], pair_r.at[k], me_z, pair)

    def x_copy(k):
        return copy(rows.at[k, 0], rows.at[k, 2], x_s.at[k], x_r.at[k], me_z, across)

    def via_copy(k):
        return copy(rows.at[k, 2], rows.at[k, 3], via_s.at[k], via_r.at[k], me_z, pair)

    def half_copy(k):
        return copy(half_out.at[k], half_in.at[k], half_s.at[k], half_r.at[k], me_z, pair)

    def cross_copy(k):
        return copy(cross_out.at[k], cross_in.at[k], cross_s.at[k], cross_r.at[k], me_z, across)

    def back_copy(k):
        return copy(final.at[k], back.at[k], back_s.at[k], back_r.at[k], flipped(me_z, k // SPLIT, spn), me_t)

    @pl.when(me_z < spn - 1)
    def _():
        halo_copy(me_z + 1).start()

    for r in range(1, tpn):
        gain_copy(r).start()
    for k, r in peers:
        meta_copy(k, r).start()
    weights[0, 0] = meta[0]
    gains[:, mine] = params[...]

    piece = min(row_count, 64)

    def convolve(first):
        total = jnp.zeros((piece, channels), f32) + params[3:4, :]
        for k in range(tap_count):
            start = first + reach - tap_count + 1 + k
            total = total + padded[start : start + piece, :] * taps[k : k + 1, :]
        block, inner = first // row_count, first % row_count
        conv[block, inner : inner + piece, :] = total.astype(bf)

    for first in range(piece, tok_rows, piece):
        convolve(first)

    @pl.when(me_z == 0)
    def _():
        padded[:reach, :] = jnp.zeros((reach, channels), f32)

    @pl.when(me_z > 0)
    def _():
        halo_copy(me_z - 1).wait_recv()

    convolve(0)
    for r in range(1, tpn):
        group_copy(r).start()
    wide[:, mine] = conv[me_t]
    for r in range(1, tpn):
        gain_copy(r).wait_recv()
    for r in range(1, tpn):
        group_copy(r).wait_recv()

    part = min(row_count, 32)
    for first in range(0, row_count, part):
        v = wide[first : first + part, :].astype(f32)
        average = jnp.sum(v, axis=1, keepdims=True) / full
        spread = jnp.sum(v * v, axis=1, keepdims=True) / full - average * average
        v = (v - average) * lax.rsqrt(spread + EPSILON) * gains[0:1, :] + gains[1:2, :]
        v = v / (1.0 + jnp.exp(-v))
        energy = jnp.sum(v * v, axis=1, keepdims=True) / full
        branch[first : first + part, :] = (v * lax.rsqrt(energy + EPSILON) * gains[2:3, :]).astype(bf)

    tile = min(hidden, 512)
    loads[0].wait()

    def project(c, power):
        cols = pl.ds(pl.multiple_of(c * tile, tile), tile)
        h = residual[:, cols].astype(f32) + jnp.dot(
            branch[...], w_out[:, cols], preferred_element_type=f32
        )
        h = h.astype(bf)
        hid[:, cols] = h
        h = h.astype(f32)
        return power + jnp.sum(h * h, axis=1, keepdims=True)

    power = lax.fori_loop(0, width // tile, project, jnp.zeros((row_count, 1), f32))
    level = lax.rsqrt(power / width + EPSILON)

    def dispatch(c, carry):
        cols = pl.ds(pl.multiple_of(c * tile, tile), tile)
        n = (hid[:, cols].astype(f32) * level * moe_gain[:, cols]).astype(bf)
        picked = jnp.dot(pick[...], n, preferred_element_type=f32).astype(bf)
        for k in range(pieces):
            send[k, :, cols] = picked[k * height : (k + 1) * height]
        return carry

    lax.fori_loop(0, width // tile, dispatch, 0)

    for k in range(SPLIT, pieces):
        z_copy(k).start()
    for k in range(SPLIT):
        rows[k, 0] = send[k]
    x_copy(0).start()
    pair_copy(0).start()
    for k, r in peers:
        meta_copy(k, r).wait_recv()
    for load in loads[1:]:
        load.wait()

    row_of, lane_of = (lax.broadcasted_iota(jnp.int32, (height, LANES), d) for d in (0, 1))

    def compute(k):
        x = rows[k].reshape(tpn * height, width)
        diagonal = lane_of == row_of + (k % SPLIT) * height
        for c in range(0, hidden, 256):
            g = jnp.dot(x, w_gate[:, c : c + 256], preferred_element_type=jnp.float32)
            u = jnp.dot(x, w_up[:, c : c + 256], preferred_element_type=jnp.float32)
            act[:, c : c + 256] = (g / (1.0 + jnp.exp(-g)) * u).astype(jnp.bfloat16)
        a = act[...]
        scales = [
            jnp.sum(jnp.where(diagonal, weights[k // SPLIT, r, pl.ds(me_t, 1), :], 0.0), axis=1, keepdims=True)
            for r in range(tpn)
        ]

        def column(c, carry):
            cols = pl.ds(pl.multiple_of(c * tile, tile), tile)
            res = jnp.dot(a, w_down[:, cols], preferred_element_type=jnp.float32).astype(jnp.bfloat16)
            res = res.astype(jnp.float32)
            parts = [res[r * height : (r + 1) * height] * scales[r] for r in range(tpn)]
            half_out[k, 0, :, cols] = parts[1].astype(jnp.bfloat16)
            half_out[k, 1, :, cols] = parts[3].astype(jnp.bfloat16)
            own[k, 0, :, cols] = parts[0]
            own[k, 1, :, cols] = parts[2]
            return carry

        lax.fori_loop(0, width // tile, column, 0)

    def step(i, carry):
        @pl.when((i + 1 >= SPLIT) & (i + 1 < pieces))
        def _():
            z_copy(i + 1).wait_recv()

        @pl.when(i + 1 < pieces)
        def _():
            k = i + 1
            x_copy(k).start()
            pair_copy(k).start()

        @pl.when(i < pieces)
        def _():
            x_copy(i).wait_recv()
            via_copy(i).start()
            pair_copy(i).wait_recv()
            via_copy(i).wait_recv()
            compute(i)
            half_copy(i).start()

        @pl.when((i >= 1) & (i <= pieces))
        def _():
            k = i - 1
            half_copy(k).wait_recv()
            cross_out[k] = (own[k, 1] + half_in[k, 1].astype(jnp.float32)).astype(jnp.bfloat16)
            cross_copy(k).start()

        @pl.when(i >= 2)
        def _():
            k = i - 2
            cross_copy(k).wait_recv()
            final[k] = (
                own[k, 0] + half_in[k, 0].astype(jnp.float32) + cross_in[k].astype(jnp.float32)
            ).astype(jnp.bfloat16)

            @pl.when(k >= SPLIT)
            def _():
                back_copy(k).start()

        return carry

    lax.fori_loop(0, pieces + 2, step, 0)
    for k in range(SPLIT):
        back[k] = final[k]
    for k in range(SPLIT, pieces):
        back_copy(k).wait_recv()

    def combine(c, carry):
        cols = pl.ds(pl.multiple_of(c * tile, tile), tile)
        total = hid[:, cols].astype(f32)
        moved = back[:, :, cols].reshape(spn * cap, tile)
        total = total + jnp.dot(unpick[...], moved, preferred_element_type=f32)
        result[:, cols] = total.astype(bf)
        return carry

    lax.fori_loop(0, width // tile, combine, 0)

    @pl.when(me_z < spn - 1)
    def _():
        halo_copy(me_z + 1).wait_send()

    for r in range(1, tpn):
        gain_copy(r).wait_send()
        group_copy(r).wait_send()
    for k, r in peers:
        meta_copy(k, r).wait_send()
    for k in range(pieces):
        for make in (x_copy, pair_copy, via_copy, half_copy, cross_copy):
            make(k).wait_send()
    for k in range(SPLIT, pieces):
        z_copy(k).wait_send()
        back_copy(k).wait_send()


def fused_layer(
    conv_value,
    conv_gate,
    kernel,
    conv_bias,
    ln_gain,
    ln_bias,
    out_gain,
    out_weight,
    residual,
    moe_gain,
    expert_ids,
    expert_weights,
    w_gate,
    w_up,
    w_down,
):
    spn, tpn = lax.axis_size("sp"), lax.axis_size("tp")
    tok_rows, channels = conv_value.shape
    row_count, width = residual.shape
    hidden = w_gate.shape[2]
    capacity = 2 * row_count // min(row_count, spn * tpn // 2)
    cap = tpn * capacity // 2
    pieces, height = spn * SPLIT, cap // SPLIT
    reach = -(-(kernel.shape[0] - 1) // SUBLANES) * SUBLANES
    bf, f32, dma = jnp.bfloat16, jnp.float32, pltpu.SemaphoreType.DMA
    vmem = pl.BlockSpec(memory_space=pltpu.VMEM)
    hbm = pl.BlockSpec(memory_space=pl.ANY)
    return pl.pallas_call(
        layer_kernel,
        out_shape=jax.ShapeDtypeStruct((row_count, width), bf),
        in_specs=[vmem] * 11 + [hbm] * 4,
        out_specs=vmem,
        scratch_shapes=[
            pltpu.VMEM(out_weight.shape, bf),
            pltpu.VMEM(w_gate.shape[1:], bf),
            pltpu.VMEM(w_up.shape[1:], bf),
            pltpu.VMEM(w_down.shape[1:], bf),
            pltpu.VMEM((reach + SUBLANES, channels), f32),
            pltpu.VMEM((SUBLANES, channels), f32),
            pltpu.VMEM((spn, SUBLANES, LANES), f32),
            pltpu.VMEM((spn * cap, row_count), bf),
            pltpu.VMEM((row_count, spn * cap), bf),
            pltpu.VMEM((reach + tok_rows, channels), f32),
            pltpu.VMEM((tpn, row_count, channels), bf),
            pltpu.VMEM((row_count, channels * tpn), bf),
            pltpu.VMEM((SUBLANES, channels * tpn), f32),
            pltpu.VMEM((row_count, channels * tpn), bf),
            pltpu.VMEM((row_count, width), bf),
            pltpu.VMEM((pieces, height, width), bf),
            pltpu.VMEM((pieces, height, width), bf),
            pltpu.VMEM((pieces, tpn, height, width), bf),
            pltpu.VMEM((spn, tpn, SUBLANES, LANES), f32),
            pltpu.VMEM((pieces, 2, height, width), f32),
            pltpu.VMEM((pieces, 2, height, width), bf),
            pltpu.VMEM((pieces, 2, height, width), bf),
            pltpu.VMEM((pieces, height, width), bf),
            pltpu.VMEM((pieces, height, width), bf),
            pltpu.VMEM((pieces, height, width), bf),
            pltpu.VMEM((tpn * height, hidden), bf),
            dma((4,)),
            dma((spn, tpn)),
            dma((spn, tpn)),
            dma((1,)),
            dma((1,)),
        ]
        + [dma((tpn,))] * 4
        + [dma((pieces,))] * 14,
        compiler_params=pltpu.CompilerParams(collective_id=0, has_side_effects=True),
    )(
        conv_value, conv_gate, kernel, conv_bias[None, :], ln_gain[None, :], ln_bias[None, :],
        out_gain[None, :], residual, moe_gain[None, :], expert_ids, expert_weights,
        out_weight, w_gate[0], w_up[0], w_down[0],
    )


def passed_along(block, axis, distance):
    devices = range(lax.axis_size(axis))
    route = [(i - distance, i) for i in devices if i - distance in devices]
    return lax.ppermute(block, axis, route)


def per_device(
    conv_value,
    conv_gate,
    kernel,
    conv_bias,
    ln_gain,
    ln_bias,
    out_gain,
    out_weight,
    residual,
    moe_gain,
    expert_ids,
    expert_weights,
    w_gate,
    w_up,
    w_down,
):
    tpn = lax.axis_size("tp")
    if lax.axis_size("sp") == GROUPS and tpn == 4:
        return fused_layer(
            conv_value, conv_gate, kernel, conv_bias, ln_gain, ln_bias, out_gain, out_weight, residual,
            moe_gain, expert_ids, expert_weights, w_gate, w_up, w_down,
        )
    tok_rows, channels = conv_value.shape
    reach_rows = kernel.shape[0] - 1
    full_channels = channels * lax.axis_size("tp")
    gated = (conv_value.astype(jnp.float32) * jax.nn.sigmoid(conv_gate.astype(jnp.float32))).astype(
        jnp.bfloat16
    )
    before = passed_along(gated[tok_rows - reach_rows :], "sp", 1)
    padded = jnp.concatenate([before, gated], axis=0)
    convolved = jnp.zeros((tok_rows, channels), jnp.float32) + conv_bias
    for offset in range(reach_rows + 1):
        convolved = convolved + padded[offset : offset + tok_rows].astype(jnp.float32) * kernel[
            offset
        ].astype(jnp.float32)
    totals = lax.psum((jnp.sum(convolved, axis=1), jnp.sum(convolved * convolved, axis=1)), "tp")
    average = (totals[0] / full_channels)[:, None]
    spread = (totals[1] / full_channels)[:, None] - average * average
    swished = jax.nn.silu((convolved - average) * lax.rsqrt(spread + EPSILON) * ln_gain + ln_bias)
    energy = lax.psum(jnp.sum(swished * swished, axis=1), "tp")
    branch = (swished * lax.rsqrt(energy / full_channels + EPSILON)[:, None] * out_gain).astype(
        jnp.bfloat16
    )
    row_count = tok_rows // lax.axis_size("tp")
    regrouped = lax.all_to_all(branch, "tp", split_axis=0, concat_axis=1, tiled=True)
    projected = jnp.dot(regrouped, out_weight, preferred_element_type=jnp.float32)
    hidden = (residual.astype(jnp.float32) + projected).astype(jnp.bfloat16)
    widened = hidden.astype(jnp.float32)
    normed = (
        widened * lax.rsqrt(jnp.mean(widened * widened, axis=1, keepdims=True) + EPSILON) * moe_gain
    ).astype(jnp.bfloat16)
    width = normed.shape[1]
    experts = lax.axis_size("sp") * lax.axis_size("tp")
    capacity = 2 * row_count // min(row_count, experts // 2)
    flat_ids = expert_ids.reshape(-1)
    onehot = (flat_ids[:, None] == jnp.arange(experts, dtype=jnp.int32)[None, :]).astype(jnp.int32)
    slot_rank = jnp.sum((jnp.cumsum(onehot, axis=0) - 1) * onehot, axis=1)
    position = flat_ids * capacity + slot_rank
    outgoing = (
        jnp.zeros((experts * capacity, width), jnp.bfloat16)
        .at[position]
        .set(jnp.repeat(normed, 2, axis=0))
    )
    outgoing = outgoing.reshape(experts, capacity, width)
    arriving = lax.all_to_all(outgoing, ("sp", "tp"), split_axis=0, concat_axis=0, tiled=True)
    flattened = arriving.reshape(-1, width)
    gate_part = jnp.dot(flattened, w_gate[0], preferred_element_type=jnp.float32)
    up_part = jnp.dot(flattened, w_up[0], preferred_element_type=jnp.float32)
    active = (jax.nn.silu(gate_part) * up_part).astype(jnp.bfloat16)
    result = jnp.dot(active, w_down[0], preferred_element_type=jnp.float32).astype(jnp.bfloat16)
    produced = result.reshape(arriving.shape)
    returned = lax.all_to_all(produced, ("sp", "tp"), split_axis=0, concat_axis=0, tiled=True)
    returned = returned.reshape(experts * capacity, width)
    picked = returned[position].reshape(row_count, 2, width)
    combined = jnp.sum(picked.astype(jnp.float32) * expert_weights[:, :, None], axis=1)
    return (widened + combined).astype(jnp.bfloat16)


def solution(mesh):
    in_specs = (
        P(("grp", "sp"), "tp"),
        P(("grp", "sp"), "tp"),
        P(None, "tp"),
        P("tp"),
        P("tp"),
        P("tp"),
        P("tp"),
        P(),
        P(("grp", "sp", "tp"), None),
        P(),
        P(("grp", "sp", "tp"), None),
        P(("grp", "sp", "tp"), None),
        P(("sp", "tp"), None, None),
        P(("sp", "tp"), None, None),
        P(("sp", "tp"), None, None),
    )
    out_specs = P(("grp", "sp", "tp"), None)
    return jax.shard_map(
        per_device, mesh=mesh, in_specs=in_specs, out_specs=out_specs, check_vma=False
    )
```

```python
import jax
import jax.numpy as jnp
from jax import lax
from jax.experimental import pallas as pl
from jax.experimental.pallas import tpu as pltpu
from jax.sharding import PartitionSpec as P

EPSILON = 1e-06
GROUPS = 4
SPLIT = 2
LANES = 128
SUBLANES = 8
MESH = pl.DeviceIdType.MESH


def flipped(index, mask, size):
    total, bit = 0, 1
    while bit < size:
        total = total + ((index // bit + mask // bit) % 2) * bit
        bit *= 2
    return total


def layer_kernel(
    value, gate, kernel, conv_bias, ln_gain, ln_bias, out_gain, residual, moe_gain, ids, shares,
    out_hbm, gate_hbm, up_hbm, down_hbm, result,
    w_out, w_gate, w_up, w_down, taps, params, meta, pick, unpick, padded, conv, wide, gains, branch, hid, send, back,
    rows, weights, own, half_out, half_in, cross_out, cross_in, final, act,
    load_sem, meta_s, meta_r, halo_s, halo_r, gain_s, gain_r, group_s, group_r,
    z_s, z_r, pair_s, pair_r, x_s, x_r, via_s, via_r,
    half_s, half_r, cross_s, cross_r, back_s, back_r,
):
    spn, tpn = weights.shape[:2]
    pieces, _, height, width = rows.shape
    cap = height * SPLIT
    me_z, me_t = lax.axis_index("sp"), lax.axis_index("tp")
    pair, across = flipped(me_t, 1, tpn), flipped(me_t, 2, tpn)
    hidden = w_gate.shape[1]
    tok_rows, channels = value.shape
    row_count = tok_rows // tpn
    full = channels * tpn
    reach = padded.shape[0] - tok_rows
    tap_count = kernel.shape[0]
    f32, bf = jnp.float32, jnp.bfloat16

    def to(z, t):
        return {"sp": z, "tp": t}

    def copy(src, dst, s, r, z, t):
        return pltpu.make_async_remote_copy(
            src_ref=src, dst_ref=dst, send_sem=s, recv_sem=r, device_id=to(z, t), device_id_type=MESH
        )

    loads = [
        pltpu.make_async_copy(a, b, load_sem.at[i])
        for i, (a, b) in enumerate(((out_hbm, w_out), (gate_hbm, w_gate), (up_hbm, w_up), (down_hbm, w_down)))
    ]
    for load in loads:
        load.start()

    peers = [(k, r) for k in range(spn) for r in range(tpn) if k or r]
    barrier = pltpu.get_barrier_semaphore()
    for k, r in peers:
        pl.semaphore_signal(
            barrier, inc=1, device_id=to(flipped(me_z, k, spn), flipped(me_t, r, tpn)), device_id_type=MESH
        )

    params[...] = jnp.zeros_like(params)
    for i, given in enumerate((ln_gain, ln_bias, out_gain, conv_bias)):
        params[i : i + 1, :] = given[...]
    taps[:tap_count, :] = kernel[...].astype(f32)

    square = (row_count, row_count)
    down, along = (lax.broadcasted_iota(jnp.int32, square, d) for d in (0, 1))

    def upright(line):
        return jnp.sum(
            jnp.where(down == along, jnp.broadcast_to(line, square), jnp.zeros((), line.dtype)),
            axis=1, keepdims=True,
        )

    group_row = jnp.broadcast_to(lax.div(ids[0:1, :], tpn), square)
    group = jnp.broadcast_to(upright(group_row[0:1, :]), square)
    same = group == group_row
    rank = jnp.sum(jnp.where(same & (along < down), 1, 0), axis=1, keepdims=True)
    rank_row = jnp.sum(jnp.where(same & (down < along), 1, 0), axis=0, keepdims=True)
    slot = jnp.bitwise_xor(group[:, 0:1], me_z) * cap + rank
    slot_row = jnp.bitwise_xor(group_row[0:1, :], me_z) * cap + rank_row
    slots = spn * cap
    pick[...] = jnp.where(
        lax.broadcasted_iota(jnp.int32, (slots, row_count), 0) == slot_row, 1.0, 0.0
    ).astype(bf)
    unpick[...] = jnp.where(
        lax.broadcasted_iota(jnp.int32, (row_count, slots), 1) == slot, 1.0, 0.0
    ).astype(bf)
    lane = lax.broadcasted_iota(jnp.int32, (row_count, LANES), 1)
    experts = lax.rem(ids[...], tpn)
    meta[...] = jnp.zeros_like(meta)
    by_expert = [
        upright(jnp.sum(jnp.where(experts == e, shares[...], 0.0), axis=0, keepdims=True))
        for e in range(tpn)
    ]
    for k in range(spn):
        here = (lane + k * cap == slot) & (lane < cap)
        for e in range(tpn):
            share = by_expert[e]
            meta[k, e : e + 1, :] = jnp.sum(jnp.where(here, share, 0.0), axis=0, keepdims=True)

    gated = value[...].astype(f32) / (1.0 + jnp.exp(-gate[...].astype(f32)))
    padded[reach:, :] = gated.astype(bf).astype(f32)
    pl.semaphore_wait(barrier, len(peers))

    mine = pl.ds(pl.multiple_of(me_t * channels, channels), channels)

    def halo_copy(z):
        return copy(
            padded.at[pl.ds(tok_rows, reach)], padded.at[pl.ds(0, reach)], halo_s.at[0], halo_r.at[0], z, me_t
        )

    def gain_copy(r):
        return copy(params, gains.at[:, mine], gain_s.at[r], gain_r.at[r], me_z, flipped(me_t, r, tpn))

    def group_copy(r):
        t = flipped(me_t, r, tpn)
        return copy(conv.at[t], wide.at[:, mine], group_s.at[r], group_r.at[r], me_z, t)

    def z_copy(k):
        return copy(send.at[k], rows.at[k, 0], z_s.at[k], z_r.at[k], flipped(me_z, k // SPLIT, spn), me_t)

    def meta_copy(k, r):
        return copy(
            meta.at[k], weights.at[k, r], meta_s.at[k, r], meta_r.at[k, r],
            flipped(me_z, k, spn), flipped(me_t, r, tpn),
        )

    def pair_copy(k):
        return copy(rows.at[k, 0], rows.at[k, 1], pair_s.at[k], pair_r.at[k], me_z, pair)

    def x_copy(k):
        return copy(rows.at[k, 0], rows.at[k, 2], x_s.at[k], x_r.at[k], me_z, across)

    def via_copy(k):
        return copy(rows.at[k, 2], rows.at[k, 3], via_s.at[k], via_r.at[k], me_z, pair)

    def half_copy(k):
        return copy(half_out.at[k], half_in.at[k], half_s.at[k], half_r.at[k], me_z, pair)

    def cross_copy(k):
        return copy(cross_out.at[k], cross_in.at[k], cross_s.at[k], cross_r.at[k], me_z, across)

    def back_copy(k):
        return copy(final.at[k], back.at[k], back_s.at[k], back_r.at[k], flipped(me_z, k // SPLIT, spn), me_t)

    @pl.when(me_z < spn - 1)
    def _():
        halo_copy(me_z + 1).start()

    for r in range(1, tpn):
        gain_copy(r).start()
    for k, r in peers:
        meta_copy(k, r).start()
    weights[0, 0] = meta[0]
    gains[:, mine] = params[...]

    piece = min(row_count, 64)

    def convolve(first):
        total = jnp.zeros((piece, channels), f32) + params[3:4, :]
        for k in range(tap_count):
            start = first + reach - tap_count + 1 + k
            total = total + padded[start : start + piece, :] * taps[k : k + 1, :]
        block, inner = first // row_count, first % row_count
        conv[block, inner : inner + piece, :] = total.astype(bf)

    for first in range(piece, tok_rows, piece):
        convolve(first)

    @pl.when(me_z == 0)
    def _():
        padded[:reach, :] = jnp.zeros((reach, channels), f32)

    @pl.when(me_z > 0)
    def _():
        halo_copy(me_z - 1).wait_recv()

    convolve(0)
    for r in range(1, tpn):
        group_copy(r).start()
    wide[:, mine] = conv[me_t]
    for r in range(1, tpn):
        gain_copy(r).wait_recv()
    for r in range(1, tpn):
        group_copy(r).wait_recv()

    part = min(row_count, 32)
    for first in range(0, row_count, part):
        v = wide[first : first + part, :].astype(f32)
        average = jnp.sum(v, axis=1, keepdims=True) / full
        spread = jnp.sum(v * v, axis=1, keepdims=True) / full - average * average
        v = (v - average) * lax.rsqrt(spread + EPSILON) * gains[0:1, :] + gains[1:2, :]
        v = v / (1.0 + jnp.exp(-v))
        energy = jnp.sum(v * v, axis=1, keepdims=True) / full
        branch[first : first + part, :] = (v * lax.rsqrt(energy + EPSILON) * gains[2:3, :]).astype(bf)

    tile = min(hidden, 512)
    loads[0].wait()

    def project(c, power):
        cols = pl.ds(pl.multiple_of(c * tile, tile), tile)
        h = residual[:, cols].astype(f32) + jnp.dot(
            branch[...], w_out[:, cols], preferred_element_type=f32
        )
        h = h.astype(bf)
        hid[:, cols] = h
        h = h.astype(f32)
        return power + jnp.sum(h * h, axis=1, keepdims=True)

    power = lax.fori_loop(0, width // tile, project, jnp.zeros((row_count, 1), f32))
    level = lax.rsqrt(power / width + EPSILON)

    def dispatch(c, carry):
        cols = pl.ds(pl.multiple_of(c * tile, tile), tile)
        n = (hid[:, cols].astype(f32) * level * moe_gain[:, cols]).astype(bf)
        picked = jnp.dot(pick[...], n, preferred_element_type=f32).astype(bf)
        for k in range(pieces):
            send[k, :, cols] = picked[k * height : (k + 1) * height]
        return carry

    lax.fori_loop(0, width // tile, dispatch, 0)

    for k in range(SPLIT, pieces):
        z_copy(k).start()
    for k in range(SPLIT):
        rows[k, 0] = send[k]
    x_copy(0).start()
    pair_copy(0).start()
    for k, r in peers:
        meta_copy(k, r).wait_recv()
    for load in loads[1:]:
        load.wait()

    row_of, lane_of = (lax.broadcasted_iota(jnp.int32, (height, LANES), d) for d in (0, 1))

    def compute(k):
        x = rows[k].reshape(tpn * height, width)
        diagonal = lane_of == row_of + (k % SPLIT) * height
        for c in range(0, hidden, 256):
            g = jnp.dot(x, w_gate[:, c : c + 256], preferred_element_type=jnp.float32)
            u = jnp.dot(x, w_up[:, c : c + 256], preferred_element_type=jnp.float32)
            act[:, c : c + 256] = (g / (1.0 + jnp.exp(-g)) * u).astype(jnp.bfloat16)
        a = act[...]
        scales = [
            jnp.sum(jnp.where(diagonal, weights[k // SPLIT, r, pl.ds(me_t, 1), :], 0.0), axis=1, keepdims=True)
            for r in range(tpn)
        ]

        def column(c, carry):
            cols = pl.ds(pl.multiple_of(c * tile, tile), tile)
            res = jnp.dot(a, w_down[:, cols], preferred_element_type=jnp.float32).astype(jnp.bfloat16)
            res = res.astype(jnp.float32)
            parts = [res[r * height : (r + 1) * height] * scales[r] for r in range(tpn)]
            half_out[k, 0, :, cols] = parts[1].astype(jnp.bfloat16)
            half_out[k, 1, :, cols] = parts[3].astype(jnp.bfloat16)
            own[k, 0, :, cols] = parts[0]
            own[k, 1, :, cols] = parts[2]
            return carry

        lax.fori_loop(0, width // tile, column, 0)

    def step(i, carry):
        @pl.when((i + 1 >= SPLIT) & (i + 1 < pieces))
        def _():
            z_copy(i + 1).wait_recv()

        @pl.when(i + 1 < pieces)
        def _():
            k = i + 1
            x_copy(k).start()
            pair_copy(k).start()

        @pl.when(i < pieces)
        def _():
            x_copy(i).wait_recv()
            via_copy(i).start()
            pair_copy(i).wait_recv()
            via_copy(i).wait_recv()
            compute(i)
            half_copy(i).start()

        @pl.when((i >= 1) & (i <= pieces))
        def _():
            k = i - 1
            half_copy(k).wait_recv()
            cross_out[k] = (own[k, 1] + half_in[k, 1].astype(jnp.float32)).astype(jnp.bfloat16)
            cross_copy(k).start()

        @pl.when(i >= 2)
        def _():
            k = i - 2
            cross_copy(k).wait_recv()
            final[k] = (
                own[k, 0] + half_in[k, 0].astype(jnp.float32) + cross_in[k].astype(jnp.float32)
            ).astype(jnp.bfloat16)

            @pl.when(k >= SPLIT)
            def _():
                back_copy(k).start()

        return carry

    lax.fori_loop(0, pieces + 2, step, 0)
    for k in range(SPLIT):
        back[k] = final[k]
    for k in range(SPLIT, pieces):
        back_copy(k).wait_recv()

    def combine(c, carry):
        cols = pl.ds(pl.multiple_of(c * tile, tile), tile)
        total = hid[:, cols].astype(f32)
        moved = back[:, :, cols].reshape(spn * cap, tile)
        total = total + jnp.dot(unpick[...], moved, preferred_element_type=f32)
        result[:, cols] = total.astype(bf)
        return carry

    lax.fori_loop(0, width // tile, combine, 0)

    @pl.when(me_z < spn - 1)
    def _():
        halo_copy(me_z + 1).wait_send()

    for r in range(1, tpn):
        gain_copy(r).wait_send()
        group_copy(r).wait_send()
    for k, r in peers:
        meta_copy(k, r).wait_send()
    for k in range(pieces):
        for make in (x_copy, pair_copy, via_copy, half_copy, cross_copy):
            make(k).wait_send()
    for k in range(SPLIT, pieces):
        z_copy(k).wait_send()
        back_copy(k).wait_send()


def fused_layer(
    conv_value,
    conv_gate,
    kernel,
    conv_bias,
    ln_gain,
    ln_bias,
    out_gain,
    out_weight,
    residual,
    moe_gain,
    expert_ids,
    expert_weights,
    w_gate,
    w_up,
    w_down,
):
    spn, tpn = lax.axis_size("sp"), lax.axis_size("tp")
    tok_rows, channels = conv_value.shape
    row_count, width = residual.shape
    hidden = w_gate.shape[2]
    capacity = 2 * row_count // min(row_count, spn * tpn // 2)
    cap = tpn * capacity // 2
    pieces, height = spn * SPLIT, cap // SPLIT
    reach = -(-(kernel.shape[0] - 1) // SUBLANES) * SUBLANES
    bf, f32, dma = jnp.bfloat16, jnp.float32, pltpu.SemaphoreType.DMA
    vmem = pl.BlockSpec(memory_space=pltpu.VMEM)
    hbm = pl.BlockSpec(memory_space=pl.ANY)
    return pl.pallas_call(
        layer_kernel,
        out_shape=jax.ShapeDtypeStruct((row_count, width), bf),
        in_specs=[vmem] * 11 + [hbm] * 4,
        out_specs=vmem,
        scratch_shapes=[
            pltpu.VMEM(out_weight.shape, bf),
            pltpu.VMEM(w_gate.shape[1:], bf),
            pltpu.VMEM(w_up.shape[1:], bf),
            pltpu.VMEM(w_down.shape[1:], bf),
            pltpu.VMEM((reach + SUBLANES, channels), f32),
            pltpu.VMEM((SUBLANES, channels), f32),
            pltpu.VMEM((spn, SUBLANES, LANES), f32),
            pltpu.VMEM((spn * cap, row_count), bf),
            pltpu.VMEM((row_count, spn * cap), bf),
            pltpu.VMEM((reach + tok_rows, channels), f32),
            pltpu.VMEM((tpn, row_count, channels), bf),
            pltpu.VMEM((row_count, channels * tpn), bf),
            pltpu.VMEM((SUBLANES, channels * tpn), f32),
            pltpu.VMEM((row_count, channels * tpn), bf),
            pltpu.VMEM((row_count, width), bf),
            pltpu.VMEM((pieces, height, width), bf),
            pltpu.VMEM((pieces, height, width), bf),
            pltpu.VMEM((pieces, tpn, height, width), bf),
            pltpu.VMEM((spn, tpn, SUBLANES, LANES), f32),
            pltpu.VMEM((pieces, 2, height, width), f32),
            pltpu.VMEM((pieces, 2, height, width), bf),
            pltpu.VMEM((pieces, 2, height, width), bf),
            pltpu.VMEM((pieces, height, width), bf),
            pltpu.VMEM((pieces, height, width), bf),
            pltpu.VMEM((pieces, height, width), bf),
            pltpu.VMEM((tpn * height, hidden), bf),
            dma((4,)),
            dma((spn, tpn)),
            dma((spn, tpn)),
            dma((1,)),
            dma((1,)),
        ]
        + [dma((tpn,))] * 4
        + [dma((pieces,))] * 14,
        compiler_params=pltpu.CompilerParams(collective_id=0, has_side_effects=True),
    )(
        conv_value, conv_gate, kernel, conv_bias[None, :], ln_gain[None, :], ln_bias[None, :],
        out_gain[None, :], residual, moe_gain[None, :], expert_ids.T, expert_weights.T,
        out_weight, w_gate[0], w_up[0], w_down[0],
    )


def passed_along(block, axis, distance):
    devices = range(lax.axis_size(axis))
    route = [(i - distance, i) for i in devices if i - distance in devices]
    return lax.ppermute(block, axis, route)


def per_device(
    conv_value,
    conv_gate,
    kernel,
    conv_bias,
    ln_gain,
    ln_bias,
    out_gain,
    out_weight,
    residual,
    moe_gain,
    expert_ids,
    expert_weights,
    w_gate,
    w_up,
    w_down,
):
    tpn = lax.axis_size("tp")
    if lax.axis_size("sp") == GROUPS and tpn == 4:
        return fused_layer(
            conv_value, conv_gate, kernel, conv_bias, ln_gain, ln_bias, out_gain, out_weight, residual,
            moe_gain, expert_ids, expert_weights, w_gate, w_up, w_down,
        )
    tok_rows, channels = conv_value.shape
    reach_rows = kernel.shape[0] - 1
    full_channels = channels * lax.axis_size("tp")
    gated = (conv_value.astype(jnp.float32) * jax.nn.sigmoid(conv_gate.astype(jnp.float32))).astype(
        jnp.bfloat16
    )
    before = passed_along(gated[tok_rows - reach_rows :], "sp", 1)
    padded = jnp.concatenate([before, gated], axis=0)
    convolved = jnp.zeros((tok_rows, channels), jnp.float32) + conv_bias
    for offset in range(reach_rows + 1):
        convolved = convolved + padded[offset : offset + tok_rows].astype(jnp.float32) * kernel[
            offset
        ].astype(jnp.float32)
    totals = lax.psum((jnp.sum(convolved, axis=1), jnp.sum(convolved * convolved, axis=1)), "tp")
    average = (totals[0] / full_channels)[:, None]
    spread = (totals[1] / full_channels)[:, None] - average * average
    swished = jax.nn.silu((convolved - average) * lax.rsqrt(spread + EPSILON) * ln_gain + ln_bias)
    energy = lax.psum(jnp.sum(swished * swished, axis=1), "tp")
    branch = (swished * lax.rsqrt(energy / full_channels + EPSILON)[:, None] * out_gain).astype(
        jnp.bfloat16
    )
    row_count = tok_rows // lax.axis_size("tp")
    regrouped = lax.all_to_all(branch, "tp", split_axis=0, concat_axis=1, tiled=True)
    projected = jnp.dot(regrouped, out_weight, preferred_element_type=jnp.float32)
    hidden = (residual.astype(jnp.float32) + projected).astype(jnp.bfloat16)
    widened = hidden.astype(jnp.float32)
    normed = (
        widened * lax.rsqrt(jnp.mean(widened * widened, axis=1, keepdims=True) + EPSILON) * moe_gain
    ).astype(jnp.bfloat16)
    width = normed.shape[1]
    experts = lax.axis_size("sp") * lax.axis_size("tp")
    capacity = 2 * row_count // min(row_count, experts // 2)
    flat_ids = expert_ids.reshape(-1)
    onehot = (flat_ids[:, None] == jnp.arange(experts, dtype=jnp.int32)[None, :]).astype(jnp.int32)
    slot_rank = jnp.sum((jnp.cumsum(onehot, axis=0) - 1) * onehot, axis=1)
    position = flat_ids * capacity + slot_rank
    outgoing = (
        jnp.zeros((experts * capacity, width), jnp.bfloat16)
        .at[position]
        .set(jnp.repeat(normed, 2, axis=0))
    )
    outgoing = outgoing.reshape(experts, capacity, width)
    arriving = lax.all_to_all(outgoing, ("sp", "tp"), split_axis=0, concat_axis=0, tiled=True)
    flattened = arriving.reshape(-1, width)
    gate_part = jnp.dot(flattened, w_gate[0], preferred_element_type=jnp.float32)
    up_part = jnp.dot(flattened, w_up[0], preferred_element_type=jnp.float32)
    active = (jax.nn.silu(gate_part) * up_part).astype(jnp.bfloat16)
    result = jnp.dot(active, w_down[0], preferred_element_type=jnp.float32).astype(jnp.bfloat16)
    produced = result.reshape(arriving.shape)
    returned = lax.all_to_all(produced, ("sp", "tp"), split_axis=0, concat_axis=0, tiled=True)
    returned = returned.reshape(experts * capacity, width)
    picked = returned[position].reshape(row_count, 2, width)
    combined = jnp.sum(picked.astype(jnp.float32) * expert_weights[:, :, None], axis=1)
    return (widened + combined).astype(jnp.bfloat16)


def solution(mesh):
    in_specs = (
        P(("grp", "sp"), "tp"),
        P(("grp", "sp"), "tp"),
        P(None, "tp"),
        P("tp"),
        P("tp"),
        P("tp"),
        P("tp"),
        P(),
        P(("grp", "sp", "tp"), None),
        P(),
        P(("grp", "sp", "tp"), None),
        P(("grp", "sp", "tp"), None),
        P(("sp", "tp"), None, None),
        P(("sp", "tp"), None, None),
        P(("sp", "tp"), None, None),
    )
    out_specs = P(("grp", "sp", "tp"), None)
    return jax.shard_map(
        per_device, mesh=mesh, in_specs=in_specs, out_specs=out_specs, check_vma=False
    )
```
